128 devices in a mesh: ep: 32 (over z, y, core), tp: 4 (over x).
Axes of the slice: x: 4, y: 4, z: 4, core: 2. Of those that a mesh axis runs over, the one named last changes fastest.
Arguments:
- conv_value: bfloat16 [49152, 2048], P(('ep', 'tp')), may hold values from -6 to 6
- conv_gate: bfloat16 [49152, 2048], P(('ep', 'tp')), may hold values from -6 to 6
- conv_taps: float32 [31, 2048], replicated, may hold values from -1 to 1
- conv_gain: float32 [2048], replicated, may hold values from 0.1 to 1.9
- conv_bias: float32 [2048], replicated, may hold values from -3 to 3
- conv_projection: bfloat16 [2048, 4096], P(None, 'tp'), may hold values from -0.125 to 0.125
- expert_input: bfloat16 [16384, 4096], P('ep'), may hold values from -6 to 6
- expert_gain: float32 [4096], replicated, may hold values from 0.1 to 1.9
- route_experts: int32 [16384, 2], P('ep'), may hold values from 0 to 31, all different within a row; in each aligned block of 128 rows (0 to 127, 128 to 255, ...) at most 16 rows name the same one
- group_gate: float32 [16384], P('ep'), may hold values from 0.3 to 1
- expert_gate: float32 [16384, 2], P('ep'), may hold values from 0.1 to 1
- gate_weight: bfloat16 [32, 4096, 1024], P('ep', None, 'tp'), may hold values from -0.09375 to 0.09375
- up_weight: bfloat16 [32, 4096, 1024], P('ep', None, 'tp'), may hold values from -0.09375 to 0.09375
- down_weight: bfloat16 [32, 1024, 4096], P('ep', None, 'tp'), may hold values from -0.1875 to 0.1875
Outputs:
- conv_out: bfloat16 [49152, 4096], P('ep', 'tp')
- expert_out: bfloat16 [16384, 4096], P('ep', 'tp')
The draws below stay inside these ranges and needn't reach their ends.
Inputs may be any that keep to these rules, and one draw needn't show every extreme that they name: `route_experts`: each row names 2 different experts; in each aligned block of 128 rows no expert is named more than 16 times, and in some blocks one expert is named exactly 16 times.
All inputs are finite; a program needn't handle non-finite values.
Results may differ from the reference program's by a relative error of at most 0.0071.
Values may be sent and summed in bfloat16 or wider, within the bound.
No kernel may reach another device: no remote copies, remote signals or barrier semaphores. Data moves between devices by JAX's collectives and lax.ppermute only.
A program may use at most 128 MiB of HBM per device.

```python
import math
import jax
import jax.numpy as jnp
import numpy as np
from jax import lax

D = 4096
CONV = 2048
KERNEL = 31
HID = 1024
EXPERTS = 32
TOP = 2
MOE_DEV = 128
CAP = 16
SEQ = 49152
MOE_ROWS = 16384


def level_of(stream_key, shape, split, low, largest):
    level = 1.0
    for position, blocks in split:
        draws = jax.random.uniform(jax.random.fold_in(jax.random.fold_in(stream_key, 6), position), (blocks,), jnp.float32, low / len(split), largest / len(split))
        level = level * jnp.repeat(jnp.exp(draws), shape[position] // blocks).reshape((-1,) + (1,) * (len(shape) - 1 - position))
    return level


def assign_block(stream_key, own, number, rows, number_of, top, limit, slope):
    sequence = jax.random.permutation(stream_key, number_of)
    crowded, common = portions_of(number_of, rows * top, limit, slope, True), portions_of(number_of, rows * top, limit, slope, False)
    places = jnp.arange(number_of)

    def named(tallies, offset_by):
        used = int((tallies > 0).sum())
        fixed = max(1, used // 4)
        passed = fixed + (places - fixed + offset_by * (used - fixed)) % max(1, number_of - fixed)
        return jnp.zeros((number_of,), jnp.int32).at[sequence[jnp.where(places < fixed, places, passed)]].set(jnp.asarray(tallies, jnp.int32))

    tallies = jnp.where(number % 4 == 0, named(crowded, number // 4), named(common, number - number // 4 - 1))
    mixed = jax.random.permutation(jax.random.fold_in(own, 3), number_of)
    donor, sink = mixed[0:number_of // 2 * 2:2], mixed[1:number_of // 2 * 2:2]
    margin = jnp.minimum(tallies[donor] - 1, limit - tallies[sink]) // 2
    margin = jnp.where((donor == sequence[0]) | (sink == sequence[0]) | (tallies[sink] == 0), 0, jnp.maximum(margin, 0))
    passed = jax.random.randint(jax.random.fold_in(own, 4), (number_of // 2,), 0, 1 << 20) % (margin + 1)
    tallies = tallies.at[donor].add(-passed).at[sink].add(passed)
    items = jnp.searchsorted(jnp.cumsum(tallies), jnp.arange(rows * top), side="right").astype(jnp.int32)
    table = items.reshape(top, rows).T
    table = table[jax.random.permutation(jax.random.fold_in(own, 1), rows)]
    offset_by = jax.random.randint(jax.random.fold_in(own, 2), (rows, 1), 0, top)
    return jnp.take_along_axis(table, (jnp.arange(top)[None, :] + offset_by) % top, axis=1)


def portions_of(count, total, bound, lean, full):
    weights = [(1 << 20) // math.isqrt(grade ** lean) + 1 for grade in range(1, count + 1)]
    largest = bound if full else min(bound, max(-(-total // count), total * weights[0] // sum(weights)))
    least = 1 if total - largest >= count - 1 else 0
    holding, rest = [largest] + [least] * (count - 1), total - largest - least * (count - 1)
    while rest > 0:
        candidates = [i for i in range(1, count) if holding[i] < largest] or [i for i in range(1, count) if holding[i] < bound]
        whole, remaining = sum([weights[i] for i in candidates]), rest
        for i in candidates:
            more = min(bound - holding[i], max(1, remaining * weights[i] // whole), rest)
            holding[i] = holding[i] + more
            rest = rest - more
    return np.array(holding)


def normal_values(rng, shape, deviation, most, shards=(), kind=jnp.bfloat16):
    level = level_of(rng, shape, shards, -0.22, 0.18) if shards else 1.0
    values = jax.random.normal(rng, shape, jnp.float32) * deviation * level
    return jnp.minimum(jnp.maximum(values, -most), most).astype(kind)


def setup_inputs(seed: int = 0) -> dict:
    splits = jax.random.split(jax.random.key(seed), 15)
    conv_value = normal_values(splits[0], (SEQ, CONV), 1.0, 6.0, ((0, 128),))
    conv_gate = normal_values(splits[1], (SEQ, CONV), 1.0, 6.0, ((0, 128),))
    conv_taps = normal_values(splits[2], (KERNEL, CONV), KERNEL ** -0.5, 1.0, (), jnp.float32)
    conv_gain = jnp.clip(1.0 + 0.18 * jax.random.normal(splits[3], (CONV,), jnp.float32), 0.1, 1.9)
    conv_bias = normal_values(splits[4], (CONV,), 0.5, 3.0, (), jnp.float32)
    conv_projection = normal_values(splits[5], (CONV, D), CONV ** -0.5, 0.125, ((1, 4),))
    expert_input = normal_values(splits[6], (MOE_ROWS, D), 1.0, 6.0, ((0, 32),))
    expert_gain = jnp.clip(1.0 + 0.18 * jax.random.normal(splits[7], (D,), jnp.float32), 0.1, 1.9)
    route_experts_keys = jax.random.split(jax.random.fold_in(splits[8], 1), MOE_ROWS // MOE_DEV)
    route_experts_turns = jax.random.permutation(jax.random.fold_in(splits[8], 3), MOE_ROWS // MOE_DEV)
    route_experts = jax.vmap(lambda own, number: assign_block(jax.random.fold_in(splits[8], 2), own, number, MOE_DEV, EXPERTS, TOP, CAP, 2))(route_experts_keys, route_experts_turns).reshape((MOE_ROWS, TOP))
    group_gate = jnp.clip(0.3 + 0.7 * jax.random.uniform(splits[9], (MOE_ROWS,), jnp.float32) ** level_of(splits[9], (MOE_ROWS,), ((0, 32),), -0.2, 0.2), 0.3, 1.0)
    expert_gate = jnp.clip(jnp.exp(math.log(1.0) - 2.3025851 * jax.random.uniform(splits[10], (MOE_ROWS, TOP), jnp.float32) ** level_of(splits[10], (MOE_ROWS, TOP), ((0, 32),), -0.2, 0.2)), 0.1, 1.0)
    gate_weight = normal_values(splits[11], (EXPERTS, D, HID), D ** -0.5, 0.09375, ((0, 32), (2, 4)))
    up_weight = normal_values(splits[12], (EXPERTS, D, HID), D ** -0.5, 0.09375, ((0, 32), (2, 4)))
    down_weight = normal_values(splits[13], (EXPERTS, HID, D), HID ** -0.5, 0.1875, ((0, 32), (2, 4)))
    return dict(conv_value=conv_value, conv_gate=conv_gate, conv_taps=conv_taps, conv_gain=conv_gain, conv_bias=conv_bias, conv_projection=conv_projection, expert_input=expert_input, expert_gain=expert_gain, route_experts=route_experts, group_gate=group_gate, expert_gate=expert_gate, gate_weight=gate_weight, up_weight=up_weight, down_weight=down_weight)


epsilon = 1e-06

def root_mean_norm(values, gain):
    widened = values.astype(jnp.float32)
    inverse_rms = lax.rsqrt(lax.optimization_barrier(jnp.mean(widened * widened, axis=-1, keepdims=True)) + epsilon)
    return (widened * inverse_rms * gain).astype(jnp.bfloat16)

def reference(conv_value, conv_gate, conv_taps, conv_gain, conv_bias, conv_projection, expert_input, expert_gain, route_experts, group_gate, expert_gate, gate_weight, up_weight, down_weight):
    gated_rows = (conv_value.astype(jnp.float32) * jax.nn.sigmoid(conv_gate.astype(jnp.float32))).astype(jnp.bfloat16)
    reach_back = KERNEL - 1
    extended = jnp.concatenate([jnp.zeros((reach_back, CONV), jnp.bfloat16), gated_rows], axis=0)
    mixed_conv = jnp.zeros((SEQ, CONV), jnp.float32)
    for lag_step in range(KERNEL):
        window = lax.slice_in_dim(extended, reach_back - lag_step, reach_back - lag_step + SEQ, axis=0)
        mixed_conv = mixed_conv + conv_taps[lag_step] * window.astype(jnp.float32)
    center = mixed_conv - lax.optimization_barrier(jnp.mean(mixed_conv, axis=-1, keepdims=True))
    spread = lax.optimization_barrier(jnp.mean(center * center, axis=-1, keepdims=True))
    activated = jax.nn.silu(center * lax.rsqrt(spread + epsilon) * conv_gain + conv_bias).astype(jnp.bfloat16)
    conv_out = jnp.dot(activated, conv_projection, preferred_element_type=jnp.float32).astype(jnp.bfloat16)
    normed = root_mean_norm(expert_input, expert_gain)
    blocks = MOE_ROWS // MOE_DEV
    picked_experts = route_experts.reshape(blocks, MOE_DEV * TOP)
    onehot = (picked_experts[:, :, None] == jnp.arange(EXPERTS, dtype=jnp.int32)[None, None, :]).astype(jnp.int32)
    before = jnp.cumsum(onehot, axis=1) - onehot
    positions = lax.optimization_barrier(jnp.sum(before * onehot, axis=2)).astype(jnp.int32)
    block_index = jnp.arange(blocks, dtype=jnp.int32)[:, None]
    token_index = block_index * MOE_DEV + jnp.arange(MOE_DEV * TOP, dtype=jnp.int32)[None, :] // TOP
    column = block_index * CAP + positions
    route_share = group_gate[:, None] * expert_gate / lax.optimization_barrier(jnp.sum(expert_gate, axis=1, keepdims=True))
    route_share = route_share.reshape(blocks, MOE_DEV * TOP)
    source = jnp.full((EXPERTS, blocks * CAP), -1, jnp.int32).at[picked_experts, column].set(token_index)
    shares = jnp.zeros((EXPERTS, blocks * CAP), jnp.float32).at[picked_experts, column].set(route_share)

    def one_expert(running, packed):
        indices, slot_shares, gate_matrix, up_matrix, down_matrix = packed
        safe_index = jnp.maximum(indices, 0)
        taken_rows = jnp.take(normed, safe_index, axis=0)
        gate_part = jnp.dot(taken_rows, gate_matrix, preferred_element_type=jnp.float32)
        up_part = jnp.dot(taken_rows, up_matrix, preferred_element_type=jnp.float32)
        hidden = (jax.nn.silu(gate_part) * up_part).astype(jnp.bfloat16)
        result = jnp.dot(hidden, down_matrix, preferred_element_type=jnp.float32).astype(jnp.bfloat16)
        return (running.at[safe_index].add(slot_shares[:, None] * result.astype(jnp.float32)), None)
    running, _ = lax.scan(one_expert, jnp.zeros((MOE_ROWS, D), jnp.float32), (source, shares, gate_weight, up_weight, down_weight))
    return (conv_out, running.astype(jnp.bfloat16))
```

```python
import functools
import jax
import jax.numpy as jnp
from jax import lax
from jax.experimental import pallas as pl
from jax.experimental.pallas import tpu as pltpu
from jax.sharding import Mesh
from jax.sharding import PartitionSpec as P

EXPERTS = 32
TOP = 2
MOE_DEV = 128
CAP = 16
PLANES = 16
CHUNKS = 2
EP_TP = ("ep_0", "ep_1", "ep_2", "tp")
EP = ("ep_0", "ep_1", "ep_2")
CHIPS = ("ep_0", "ep_1")
CORE_TP = ("ep_2", "tp")

epsilon = 1e-06
f32 = jnp.float32
bf16 = jnp.bfloat16


def ring_pairs(move):
    pairs = []
    for core in range(2):
        for x in range(4):
            to_core, to_x = move(core, x)
            pairs.append((core * 4 + x, to_core * 4 + to_x))
    return pairs


def weight_partner(core, x):
    return core, (((x - core) % 4 ^ 1) + core) % 4


def hidden_partner(core, x):
    return core, ((3 - (x - core) % 4) + core) % 4


def other_core(core, x):
    return 1 - core, x


def diagonal(core, x):
    return 1 - core, weight_partner(core, x)[1]


def swapped(value, move):
    return lax.ppermute(value, CORE_TP, ring_pairs(move))


def block_slots(info, core):
    picks = info[:, 0:TOP].astype(jnp.int32)
    first, second = picks[:, 0:1], picks[:, 1:2]
    rows = info.shape[0]
    lanes = lax.broadcasted_iota(jnp.int32, (rows, EXPERTS), 1)
    in_first, in_second = first == lanes, second == lanes
    named = jnp.where(in_first | in_second, 1.0, 0.0).astype(bf16)
    earlier = (
        lax.broadcasted_iota(jnp.int32, (rows, rows), 1)
        < lax.broadcasted_iota(jnp.int32, (rows, rows), 0)
    )
    before = jnp.dot(
        jnp.where(earlier, 1.0, 0.0).astype(bf16), named, preferred_element_type=f32
    )
    slots = []
    for pick, mask in ((first, in_first), (second, in_second)):
        position = jnp.sum(jnp.where(mask, before, 0.0), axis=1, keepdims=True)
        slot = (pick >> 1) * CAP + position.astype(jnp.int32)
        slots.append(jnp.where((pick & 1) == core, slot, -1))
    return slots


def dispatch_kernel(where, own_ref, sib_ref, own_info, sib_info, gain_ref, out_ref):
    core = where[1]
    gain = gain_ref[...]
    width = 512

    def run(x_ref, info_ref):
        widened = x_ref[...].astype(f32)
        depth = widened.shape[1]
        inverse = lax.rsqrt(jnp.mean(widened * widened, axis=-1, keepdims=True) + epsilon)
        slot_a, slot_b = block_slots(info_ref[...], core)
        lanes = lax.broadcasted_iota(jnp.int32, (MOE_DEV, PLANES * CAP), 1)
        table = jnp.where((lanes == slot_a) | (lanes == slot_b), 1.0, 0.0)
        spread = table.T.astype(bf16)
        for k in range(depth // width):
            cols = slice(k * width, (k + 1) * width)
            normed = (x_ref[:, cols].astype(f32) * inverse * gain[:, cols]).astype(bf16)
            rows = jnp.dot(spread, normed, preferred_element_type=f32).astype(bf16)
            out_ref[:, :, cols] = rows.reshape(PLANES, CAP, width)

    @pl.when(pl.program_id(0) == 0)
    def _():
        run(own_ref, own_info)

    @pl.when(pl.program_id(0) == 1)
    def _():
        run(sib_ref, sib_info)


def dispatch(where, expert_input, sib_rows, info, sib_info, gain, chunk):
    depth = expert_input.shape[1]
    per_half = 2
    return pl.pallas_call(
        dispatch_kernel,
        grid_spec=pltpu.PrefetchScalarGridSpec(
            num_scalar_prefetch=1,
            grid=(2,),
            in_specs=[
                pl.BlockSpec((MOE_DEV, depth), lambda i, w: (w[0] * per_half + chunk, 0)),
                pl.BlockSpec((MOE_DEV, depth), lambda i, w: (chunk, 0)),
                pl.BlockSpec((MOE_DEV, 4), lambda i, w: (w[0] * per_half + chunk, 0)),
                pl.BlockSpec((MOE_DEV, 4), lambda i, w: (w[0] * per_half + chunk, 0)),
                pl.BlockSpec((1, depth), lambda i, w: (0, 0)),
            ],
            out_specs=pl.BlockSpec((PLANES, CAP, depth), lambda i, w: (0, i, 0)),
        ),
        out_shape=jax.ShapeDtypeStruct((PLANES, 2 * CAP, depth), bf16),
        cost_estimate=pl.CostEstimate(
            flops=2 * 2 * MOE_DEV * PLANES * CAP * depth * 8,
            bytes_accessed=8 << 20,
            transcendentals=0,
        ),
        name="dispatch",
    )(where, expert_input, sib_rows, info, sib_info, gain)


def combine_kernel(where, own_info, sib_info, result_ref, keep, to_partner, to_sib, to_diag):
    core = where[1]
    half = keep.shape[1]
    for source, info_ref in enumerate((own_info, sib_info)):
        info = info_ref[...]
        slot_a, slot_b = block_slots(info, core)
        lanes = lax.broadcasted_iota(jnp.int32, (MOE_DEV, PLANES * CAP), 1)
        weights = jnp.where(lanes == slot_a, info[:, 2:3], 0.0) + jnp.where(
            lanes == slot_b, info[:, 3:4], 0.0
        )
        coarse = weights.astype(bf16)
        fine = (weights - coarse.astype(f32)).astype(bf16)
        for part in range(2):
            table = result_ref[
                :, source * CAP : (source + 1) * CAP, part * half : (part + 1) * half
            ].reshape(PLANES * CAP, half)
            total = jnp.dot(coarse, table, preferred_element_type=f32) + jnp.dot(
                fine, table, preferred_element_type=f32
            )
            ref = ((keep, to_partner), (to_sib, to_diag))[source][part]
            ref[...] = total.astype(ref.dtype)


def combine(where, info, sib_info, returned, chunk):
    half = returned.shape[2] // 2
    per_half = 2
    whole = lambda i, w: (0, 0)
    shapes = [jax.ShapeDtypeStruct((MOE_DEV, half), t) for t in (f32, bf16, bf16, bf16)]
    return pl.pallas_call(
        combine_kernel,
        grid_spec=pltpu.PrefetchScalarGridSpec(
            num_scalar_prefetch=1,
            grid=(1,),
            in_specs=[
                pl.BlockSpec((MOE_DEV, 4), lambda i, w: (w[0] * per_half + chunk, 0)),
                pl.BlockSpec((MOE_DEV, 4), lambda i, w: (w[0] * per_half + chunk, 0)),
                pl.BlockSpec(returned.shape, lambda i, w: (0, 0, 0)),
            ],
            out_specs=[pl.BlockSpec((MOE_DEV, half), whole)] * 4,
        ),
        out_shape=shapes,
        cost_estimate=pl.CostEstimate(
            flops=4 << 30, bytes_accessed=4 << 20, transcendentals=0
        ),
        name="combine",
    )(where, info, sib_info, returned)


def conv_rows(conv_value, conv_gate, conv_taps, conv_gain, conv_bias):
    gated_rows = (
        conv_value.astype(f32) * jax.nn.sigmoid(conv_gate.astype(f32))
    ).astype(bf16)
    reach_back = conv_taps.shape[0] - 1
    length = gated_rows.shape[0]
    count = lax.axis_size(EP_TP)
    earlier = lax.ppermute(
        gated_rows[length - reach_back :], EP_TP, [(k, k + 1) for k in range(count - 1)]
    )
    extended = jnp.concatenate([earlier, gated_rows], axis=0)
    mixed = jnp.zeros(gated_rows.shape, f32)
    for lag in range(reach_back + 1):
        window = lax.slice_in_dim(extended, reach_back - lag, reach_back - lag + length, axis=0)
        mixed = mixed + conv_taps[lag] * window.astype(f32)
    center = mixed - jnp.mean(mixed, axis=-1, keepdims=True)
    spread = jnp.mean(center * center, axis=-1, keepdims=True)
    return jax.nn.silu(center * lax.rsqrt(spread + epsilon) * conv_gain + conv_bias).astype(bf16)


def on_device(
    conv_value,
    conv_gate,
    conv_taps,
    conv_gain,
    conv_bias,
    conv_projection,
    expert_input,
    expert_gain,
    route_experts,
    group_gate,
    expert_gate,
    gate_weight,
    up_weight,
    down_weight,
):
    core, x = lax.axis_index("ep_2"), lax.axis_index("tp")
    place = (x - core) % 4

    def half_of(which_core):
        spot = (x - which_core) % 4
        return ((spot == 1) | (spot == 2)).astype(jnp.int32)

    half, sib_half = half_of(core), half_of(1 - core)
    where = jnp.stack([half, core]).astype(jnp.int32)
    rows_half = expert_input.shape[0] // 2

    gate_own, up_own, down_own = gate_weight[0], up_weight[0], down_weight[0]

    outgoing = lax.dynamic_slice_in_dim(expert_input, sib_half * rows_half, rows_half, 0)
    share = group_gate[:, None] * expert_gate / jnp.sum(expert_gate, axis=1, keepdims=True)
    info = jnp.concatenate([route_experts.astype(f32), share], axis=1)
    sib_rows = swapped(outgoing, other_core)
    sib_info = swapped(info, other_core)
    gate_part = swapped(gate_own, weight_partner)
    up_part = swapped(up_own, weight_partner)
    gain = expert_gain[None]

    sends = [
        dispatch(where, expert_input, sib_rows, info, sib_info, gain, k) for k in range(CHUNKS)
    ]
    arrived = [
        lax.all_to_all(s, CHIPS, split_axis=0, concat_axis=0, tiled=True) for s in sends
    ]

    conv_value, conv_gate, _ = lax.optimization_barrier((conv_value, conv_gate, sends[0]))
    activated = conv_rows(conv_value, conv_gate, conv_taps, conv_gain, conv_bias)
    down_part = swapped(down_own, weight_partner)

    hidden_order = [place, place ^ 1, 3 - place, (3 - place) ^ 1]
    quarter = down_own.shape[0] // 4

    def ordered(matrix):
        return jnp.concatenate(
            [
                lax.dynamic_slice_in_dim(matrix, (p + core) % 4 * quarter, quarter, 0)
                for p in hidden_order
            ],
            axis=0,
        )

    down_all = jnp.concatenate([ordered(down_own), ordered(down_part)], axis=1)
    near, far = down_all[: 2 * quarter], down_all[2 * quarter :]

    pieces = []
    for k in range(CHUNKS):
        tokens = arrived[k].reshape(-1, arrived[k].shape[2])
        parts = []
        for gate_matrix, up_matrix in ((gate_own, up_own), (gate_part, up_part)):
            gate_out = jnp.dot(tokens, gate_matrix, preferred_element_type=f32)
            up_out = jnp.dot(tokens, up_matrix, preferred_element_type=f32)
            parts.append((jax.nn.silu(gate_out) * up_out).astype(bf16))
        hidden = jnp.concatenate(parts, axis=1)
        other = swapped(hidden, hidden_partner)
        summed = jnp.dot(hidden, near, preferred_element_type=f32)
        summed = summed + jnp.dot(other, far, preferred_element_type=f32)
        result = summed.astype(bf16).reshape(PLANES, 2 * CAP, -1)
        returned = lax.all_to_all(result, CHIPS, split_axis=0, concat_axis=0, tiled=True)
        keep, to_partner, to_sib, to_diag = combine(where, info, sib_info, returned, k)
        from_partner = swapped(to_partner, weight_partner)
        from_sib = swapped(to_sib, other_core)
        from_diag = swapped(to_diag, diagonal)
        mine = jnp.stack([keep, from_partner.astype(f32)])
        mine = jnp.where(half == 0, mine, mine[::-1])
        theirs = jnp.stack([from_sib.astype(f32), from_diag.astype(f32)])
        theirs = jnp.where(sib_half == 0, theirs, theirs[::-1])
        pieces.append((mine + theirs).astype(bf16))
    expert_out = jnp.stack(pieces, axis=1).reshape(expert_input.shape[0], -1)

    rows = activated.shape[0]
    middle = rows // 2
    right = [(k, (k + 1) % 4) for k in range(4)]
    left = [(k, (k - 1) % 4) for k in range(4)]
    from_left = lax.ppermute(activated, "tp", right)
    from_right = lax.ppermute(activated, "tp", left)
    far_top = lax.ppermute(from_left[:middle], "tp", right)
    far_bottom = lax.ppermute(from_right[middle:], "tp", left)
    conv_out = jnp.zeros((4 * rows, conv_projection.shape[1]), bf16)
    for block, offset, start in (
        (activated, 0, 0),
        (from_left, 3, 0),
        (from_right, 1, 0),
        (far_top, 2, 0),
        (far_bottom, 2, middle),
    ):
        product = jnp.dot(block, conv_projection, preferred_element_type=f32).astype(bf16)
        conv_out = lax.dynamic_update_slice_in_dim(
            conv_out, product, (x + offset) % 4 * rows + start, 0
        )
    return (conv_out, expert_out)


def solution(mesh):
    finer = Mesh(mesh.devices.reshape(4, 4, 2, mesh.shape["tp"]), EP_TP)
    in_specs = (
        P(EP_TP, None),
        P(EP_TP, None),
        P(),
        P(),
        P(),
        P(None, "tp"),
        P(EP, None),
        P(),
        P(EP, None),
        P(EP),
        P(EP, None),
        P(EP, None, "tp"),
        P(EP, None, "tp"),
        P(EP, None, "tp"),
    )
    out_specs = (P(EP, "tp"), P(EP, "tp"))
    return jax.shard_map(
        on_device, mesh=finer, in_specs=in_specs, out_specs=out_specs, check_vma=False
    )
```

```python
import jax
import jax.numpy as jnp
from jax import lax
from jax.experimental import pallas as pl
from jax.experimental.pallas import tpu as pltpu
from jax.sharding import Mesh
from jax.sharding import PartitionSpec as P

EXPERTS = 32
TOP = 2
MOE_DEV = 128
CAP = 16
PLANES = 16
CHUNKS = 2
EP_TP = ("ep_0", "ep_1", "ep_2", "tp")
EP = ("ep_0", "ep_1", "ep_2")
CHIPS = ("ep_0", "ep_1")
CORE_TP = ("ep_2", "tp")

epsilon = 1e-06
f32 = jnp.float32
bf16 = jnp.bfloat16


def ring_pairs(move):
    pairs = []
    for core in range(2):
        for x in range(4):
            to_core, to_x = move(core, x)
            pairs.append((core * 4 + x, to_core * 4 + to_x))
    return pairs


def weight_partner(core, x):
    return core, (((x - core) % 4 ^ 1) + core) % 4


def hidden_partner(core, x):
    return core, ((3 - (x - core) % 4) + core) % 4


def other_core(core, x):
    return 1 - core, x


def diagonal(core, x):
    return 1 - core, weight_partner(core, x)[1]


def swapped(value, move):
    return lax.ppermute(value, CORE_TP, ring_pairs(move))


def exchanged(blocks):
    return lax.all_to_all(blocks, CHIPS, split_axis=0, concat_axis=0, tiled=True)


def params(mib):
    return pltpu.CompilerParams(vmem_limit_bytes=mib << 20)


def cost(microseconds, mib):
    return pl.CostEstimate(
        flops=int(microseconds * 7e8), bytes_accessed=mib << 20, transcendentals=0
    )


def block_slots(info, core):
    picks = info[0:TOP, :].astype(jnp.int32)
    first, second = picks[0:1, :], picks[1:2, :]
    count = info.shape[1]
    experts = lax.broadcasted_iota(jnp.int32, (EXPERTS, count), 0)
    in_first, in_second = first == experts, second == experts
    named = jnp.where(in_first | in_second, 1.0, 0.0).astype(bf16)
    earlier = (
        lax.broadcasted_iota(jnp.int32, (count, count), 0)
        < lax.broadcasted_iota(jnp.int32, (count, count), 1)
    )
    before = jnp.dot(
        named, jnp.where(earlier, 1.0, 0.0).astype(bf16), preferred_element_type=f32
    )
    slots = []
    for pick, mask in ((first, in_first), (second, in_second)):
        position = jnp.sum(jnp.where(mask, before, 0.0), axis=0, keepdims=True)
        slot = (pick >> 1) * CAP + position.astype(jnp.int32)
        slots.append(jnp.where((pick & 1) == core, slot, -1))
    return slots


def dispatch_kernel(where, x_ref, info_ref, gain_ref, out_ref):
    width = 1024
    widened = x_ref[...].astype(f32)
    inverse = lax.rsqrt(jnp.mean(widened * widened, axis=-1, keepdims=True) + epsilon)
    slot_a, slot_b = block_slots(info_ref[...], where[1])
    slots = lax.broadcasted_iota(jnp.int32, (PLANES * CAP, MOE_DEV), 0)
    spread = jnp.where((slots == slot_a) | (slots == slot_b), 1.0, 0.0).astype(bf16)

    depth = out_ref.shape[2]
    first = 0 if depth == x_ref.shape[1] else where[7] * depth

    def piece(k, carry):
        cols = pl.ds(pl.multiple_of(first + k * width, width), width)
        normed = (x_ref[:, cols].astype(f32) * inverse * gain_ref[:, cols]).astype(bf16)
        rows = jnp.dot(spread, normed, preferred_element_type=f32).astype(bf16)
        out_ref[:, :, pl.ds(pl.multiple_of(k * width, width), width)] = rows.reshape(
            PLANES, CAP, width
        )
        return carry

    lax.fori_loop(0, depth // width, piece, 0)


def dispatch(where, rows, info, gain, whole_rows, out_depth):
    depth = rows.shape[1]
    row_block = lambda i, w: (w[0] * 2 + i, 0)
    return pl.pallas_call(
        dispatch_kernel,
        grid_spec=pltpu.PrefetchScalarGridSpec(
            num_scalar_prefetch=1,
            grid=(2,),
            in_specs=[
                pl.BlockSpec((MOE_DEV, depth), row_block if whole_rows else lambda i, w: (i, 0)),
                pl.BlockSpec((info.shape[0], MOE_DEV), lambda i, w: (0, w[0] * 2 + i)),
                pl.BlockSpec((1, depth), lambda i, w: (0, 0)),
            ],
            out_specs=pl.BlockSpec((PLANES, CAP, out_depth), lambda i, w: (0, i, 0)),
        ),
        out_shape=jax.ShapeDtypeStruct((PLANES, 2 * CAP, out_depth), bf16),
        cost_estimate=cost(6, 6),
        name="dispatch",
    )(where, rows, info, gain)


def hidden_kernel(where, low, high, gate_own, up_own, gate_part, up_part, out_ref, totals):
    step, steps = pl.program_id(0), pl.num_programs(0)
    width = gate_own.shape[1]

    @pl.when(step == 0)
    def _():
        totals[...] = jnp.zeros_like(totals)

    def add(block):
        for i, ref in enumerate((gate_own, up_own, gate_part, up_part)):
            totals[i] += jnp.dot(block, ref[...], preferred_element_type=f32)

    @pl.when(step < steps // 2)
    def _():
        add(low[...])

    @pl.when(step >= steps // 2)
    def _():
        add(high[...])

    @pl.when(step == steps - 1)
    def _():
        for i in range(2):
            value = jax.nn.silu(totals[2 * i]) * totals[2 * i + 1]
            out_ref[:, i * width : (i + 1) * width] = value.astype(bf16)


def hidden_units(where, low, high, gate_own, up_own, gate_part, up_part):
    depth, width = gate_own.shape
    rows = low.shape[0]
    step = 1024
    half = depth // step // 2
    if low is high:
        order = lambda k, w: k
        high_block = lambda k, w: (0, jnp.maximum(k, half))
    else:
        order = lambda k, w: lax.rem(k + w[7] * half, 2 * half)
        high_block = lambda k, w: (0, jnp.maximum(k - half, 0))
    weight = pl.BlockSpec((step, width), lambda k, w: (order(k, w), 0))
    return pl.pallas_call(
        hidden_kernel,
        grid_spec=pltpu.PrefetchScalarGridSpec(
            num_scalar_prefetch=1,
            grid=(2 * half,),
            in_specs=[
                pl.BlockSpec((rows, step), lambda k, w: (0, jnp.minimum(k, half - 1))),
                pl.BlockSpec((rows, step), high_block),
            ]
            + [weight] * 4,
            out_specs=pl.BlockSpec((rows, 2 * width), lambda k, w: (0, 0)),
            scratch_shapes=[pltpu.VMEM((4, rows, width), f32)],
        ),
        out_shape=jax.ShapeDtypeStruct((rows, 2 * width), bf16),
        cost_estimate=cost(10, 12),
        name="hidden",
    )(where, low, high, gate_own, up_own, gate_part, up_part)


def down_kernel(where, near, far, own_ref, part_ref, out_ref):
    quarter = near.shape[1] // 2

    def run(weight):
        total = None
        for i in range(4):
            source = (near, far)[i // 2]
            values = source[:, (i % 2) * quarter : (i % 2 + 1) * quarter]
            rows = pl.ds(pl.multiple_of(where[2 + i] * quarter, quarter), quarter)
            product = jnp.dot(values, weight[rows, :], preferred_element_type=f32)
            total = product if total is None else total + product
        out_ref[...] = total.astype(bf16).reshape(out_ref.shape)

    @pl.when(pl.program_id(0) < 2)
    def _():
        run(own_ref)

    @pl.when(pl.program_id(0) >= 2)
    def _():
        run(part_ref)


def down_result(where, near, far, down_own, down_part):
    rows = near.shape[0]
    depth, width = down_own.shape
    step = width // 2
    whole = pl.BlockSpec(near.shape, lambda j, w: (0, 0))
    return pl.pallas_call(
        down_kernel,
        grid_spec=pltpu.PrefetchScalarGridSpec(
            num_scalar_prefetch=1,
            grid=(4,),
            in_specs=[
                whole,
                whole,
                pl.BlockSpec((depth, step), lambda j, w: (0, jnp.minimum(j, 1))),
                pl.BlockSpec((depth, step), lambda j, w: (0, jnp.maximum(j - 2, 0))),
            ],
            out_specs=pl.BlockSpec((PLANES, rows // PLANES, step), lambda j, w: (0, 0, j)),
        ),
        out_shape=jax.ShapeDtypeStruct((PLANES, rows // PLANES, 2 * width), bf16),
        cost_estimate=cost(5, 7),
        name="down",
    )(where, near, far, down_own, down_part)


def combine_kernel(where, info_ref, result_ref, own_slice, other_slice):
    half = own_slice.shape[1]
    info = info_ref[...]
    slot_a, slot_b = block_slots(info, where[1])
    slots = lax.broadcasted_iota(jnp.int32, (PLANES * CAP, MOE_DEV), 0)
    weights = jnp.where(slots == slot_a, info[2:3, :], 0.0) + jnp.where(
        slots == slot_b, info[3:4, :], 0.0
    )
    coarse = weights.astype(bf16)
    fine = weights - coarse.astype(f32)
    table = jnp.concatenate([coarse.astype(f32).T, fine.T], axis=0).astype(bf16)
    for part, ref in enumerate((own_slice, other_slice)):
        rows = result_ref[:, :, part * half : (part + 1) * half].reshape(PLANES * CAP, half)
        total = jnp.dot(table, rows, preferred_element_type=f32)
        ref[...] = (total[:MOE_DEV] + total[MOE_DEV:]).astype(ref.dtype)


def combine(where, info, returned, own_type):
    half = returned.shape[2] // 2
    out = pl.BlockSpec((MOE_DEV, half), lambda i, w: (i, 0))
    return pl.pallas_call(
        combine_kernel,
        grid_spec=pltpu.PrefetchScalarGridSpec(
            num_scalar_prefetch=1,
            grid=(2,),
            in_specs=[
                pl.BlockSpec((4, MOE_DEV), lambda i, w: (0, w[0] * 2 + i)),
                pl.BlockSpec((PLANES, CAP, 2 * half), lambda i, w: (0, i, 0)),
            ],
            out_specs=[out, out],
        ),
        out_shape=[jax.ShapeDtypeStruct((2 * MOE_DEV, half), t) for t in (own_type, bf16)],
        cost_estimate=cost(4, 4),
        compiler_params=params(12),
        name="combine",
    )(where, info, returned)


def total_kernel(where, keep, partner, sib, diag, out_ref):
    half = pl.program_id(0)

    def add(mine, theirs):
        out_ref[...] = (mine[...].astype(f32) + theirs[...].astype(f32)).astype(bf16)

    for own_place in range(2):
        for sib_place in range(2):

            @pl.when(((half == where[0]) == (own_place == 0)) & ((half == where[6]) == (sib_place == 0)))
            def _():
                add((keep, partner)[own_place], (sib, diag)[sib_place])


def total_rows(where, keep, partner, sib, diag):
    rows, width = keep.shape
    whole = pl.BlockSpec((rows, width), lambda i, w: (0, 0))
    return pl.pallas_call(
        total_kernel,
        grid_spec=pltpu.PrefetchScalarGridSpec(
            num_scalar_prefetch=1,
            grid=(2,),
            in_specs=[whole] * 4,
            out_specs=pl.BlockSpec((rows, width), lambda i, w: (i, 0)),
        ),
        out_shape=jax.ShapeDtypeStruct((2 * rows, width), bf16),
        cost_estimate=cost(3, 4),
        compiler_params=params(12),
        name="total",
    )(where, keep, partner, sib, diag)


def gated_rows(value, gate):
    return (value.astype(f32) * jax.nn.sigmoid(gate.astype(f32))).astype(bf16)


def conv_kernel(
    value_ref, gate_ref, halo_ref, taps_ref, gain_ref, bias_ref, top_ref, bottom_ref, rows, mixed
):
    reach = halo_ref.shape[0]
    block = value_ref.shape[0]
    lanes = 128

    @pl.when(pl.program_id(0) == 0)
    def _():
        rows[:reach, :] = halo_ref[...].astype(f32)

    @pl.when(pl.program_id(0) > 0)
    def _():
        rows[:reach, :] = rows[block:, :]

    rows[reach:, :] = gated_rows(value_ref[...], gate_ref[...]).astype(f32)

    def piece(k, carry):
        cols = pl.ds(pl.multiple_of(k * lanes, lanes), lanes)
        column = rows[:, cols]
        total = jnp.zeros((block, lanes), f32)
        for phase in range(8):
            moved = column if phase == 0 else pltpu.roll(column, phase, 0)
            for lag in range(phase, taps_ref.shape[0], 8):
                start = reach - (lag - phase)
                total = total + taps_ref[lag : lag + 1, cols] * moved[start : start + block]
        mixed[:, cols] = total
        return carry

    lax.fori_loop(0, mixed.shape[1] // lanes, piece, 0)
    whole = mixed[...]
    center = whole - jnp.mean(whole, axis=-1, keepdims=True)
    spread = jnp.mean(center * center, axis=-1, keepdims=True)
    scaled = center * lax.rsqrt(spread + epsilon) * gain_ref[...] + bias_ref[...]
    result = jax.nn.silu(scaled).astype(bf16)
    half = pl.num_programs(0) // 2

    @pl.when(pl.program_id(0) < half)
    def _():
        top_ref[...] = result

    @pl.when(pl.program_id(0) >= half)
    def _():
        bottom_ref[...] = result


def conv_rows(conv_value, conv_gate, earlier, conv_taps, conv_gain, conv_bias):
    length, width = conv_value.shape
    block = 64
    half = length // block // 2
    reach = earlier.shape[0]
    row_block = pl.BlockSpec((block, width), lambda i: (i, 0))
    whole = lambda rows: pl.BlockSpec((rows, width), lambda i: (0, 0))
    return pl.pallas_call(
        conv_kernel,
        grid=(length // block,),
        in_specs=[row_block, row_block, whole(reach), whole(conv_taps.shape[0]), whole(1), whole(1)],
        out_specs=[
            pl.BlockSpec((block, width), lambda i: (jnp.minimum(i, half - 1), 0)),
            pl.BlockSpec((block, width), lambda i: (jnp.maximum(i - half, 0), 0)),
        ],
        out_shape=[jax.ShapeDtypeStruct((length // 2, width), bf16)] * 2,
        scratch_shapes=[
            pltpu.VMEM((reach + block, width), f32),
            pltpu.VMEM((block, width), f32),
        ],
        cost_estimate=cost(14, 5),
        compiler_params=params(12),
    )(conv_value, conv_gate, earlier, conv_taps, conv_gain[None], conv_bias[None])


def work(
    conv_value,
    conv_gate,
    conv_taps,
    conv_gain,
    conv_bias,
    conv_projection,
    expert_input,
    expert_gain,
    route_experts,
    group_gate,
    expert_gate,
    gate_weight,
    up_weight,
    down_weight,
):
    core, x = lax.axis_index("ep_2"), lax.axis_index("tp")
    place = (x - core) % 4

    def half_of(which_core):
        spot = (x - which_core) % 4
        return ((spot == 1) | (spot == 2)).astype(jnp.int32)

    half, sib_half = half_of(core), half_of(1 - core)
    hidden_order = [place, place ^ 1, 3 - place, (3 - place) ^ 1]
    quarters = [(p + core) % 4 for p in hidden_order]
    where = jnp.stack([half, core, *quarters, sib_half, place >> 1]).astype(jnp.int32)
    rows_half = expert_input.shape[0] // 2
    gate_own, up_own, down_own = gate_weight[0], up_weight[0], down_weight[0]
    gain = expert_gain[None]

    outgoing = lax.dynamic_slice_in_dim(expert_input, sib_half * rows_half, rows_half, 0)
    sib_rows = swapped(outgoing, other_core)
    share = group_gate[:, None] * expert_gate / jnp.sum(expert_gate, axis=1, keepdims=True)
    info = jnp.concatenate([route_experts.astype(f32).T, share.T], axis=0)
    sib_info = swapped(info, other_core)
    gate_part = swapped(gate_own, weight_partner)
    up_part = swapped(up_own, weight_partner)

    infos = (info, sib_info)
    depth = expert_input.shape[1]
    first = dispatch(where, expert_input, route_experts.T, gain, True, depth // 2)
    first_arrived = exchanged(first)
    second = dispatch(where, sib_rows, sib_info, gain, False, depth)
    second, first_arrived = lax.optimization_barrier((second, first_arrived))
    second_arrived = exchanged(second).reshape(-1, depth)
    low = first_arrived.reshape(-1, depth // 2)
    high = swapped(low, hidden_partner)
    arrived = ((low, high), (second_arrived, second_arrived))

    reach = 32
    tail = gated_rows(conv_value[-reach:], conv_gate[-reach:])
    count = lax.axis_size(EP_TP)
    earlier = lax.ppermute(tail, EP_TP, [(k, k + 1) for k in range(count - 1)])
    conv_value, conv_gate, _ = lax.optimization_barrier((conv_value, conv_gate, first))
    top, bottom = conv_rows(
        conv_value, conv_gate, earlier, conv_taps, conv_gain, conv_bias
    )
    down_part = swapped(down_own, weight_partner)

    combined = []
    for k in range(CHUNKS):
        near = hidden_units(where, *arrived[k], gate_own, up_own, gate_part, up_part)
        far = swapped(near, hidden_partner)
        result = down_result(where, near, far, down_own, down_part)
        returned = exchanged(result)
        combined.append(combine(where, infos[k], returned, (f32, bf16)[k]))
    keep, from_partner = combined[0][0], swapped(combined[0][1], weight_partner)
    from_sib = swapped(combined[1][0], other_core)
    from_diag = swapped(combined[1][1], diagonal)
    expert_out = total_rows(where, keep, from_partner, from_sib, from_diag)

    rows = conv_value.shape[0]
    middle = rows // 2
    right = [(k, (k + 1) % 4) for k in range(4)]
    left = [(k, (k - 1) % 4) for k in range(4)]

    def passed(value, pairs):
        return lax.ppermute(value, "tp", pairs)

    left_top = passed(top, right)
    right_bottom = passed(bottom, left)
    left_bottom = passed(bottom, right)
    right_top = passed(top, left)
    far_top = passed(left_top, right)
    far_bottom = passed(right_bottom, left)
    conv_out = jnp.zeros((4 * rows, conv_projection.shape[1]), bf16)
    for block, offset, start in (
        (top, 0, 0),
        (bottom, 0, middle),
        (left_top, 3, 0),
        (right_bottom, 1, middle),
        (left_bottom, 3, middle),
        (right_top, 1, 0),
        (far_top, 2, 0),
        (far_bottom, 2, middle),
    ):
        product = jnp.dot(block, conv_projection, preferred_element_type=f32).astype(bf16)
        conv_out = lax.dynamic_update_slice_in_dim(
            conv_out, product, (x + offset) % 4 * rows + start, 0
        )
    return (conv_out, expert_out)


def solution(mesh):
    finer = Mesh(mesh.devices.reshape(4, 4, 2, mesh.shape["tp"]), EP_TP)
    in_specs = (
        P(EP_TP, None),
        P(EP_TP, None),
        P(),
        P(),
        P(),
        P(None, "tp"),
        P(EP, None),
        P(),
        P(EP, None),
        P(EP),
        P(EP, None),
        P(EP, None, "tp"),
        P(EP, None, "tp"),
        P(EP, None, "tp"),
    )
    out_specs = (P(EP, "tp"), P(EP, "tp"))
    return jax.shard_map(work, mesh=finer, in_specs=in_specs, out_specs=out_specs, check_vma=False)
```

```python
import jax
import jax.numpy as jnp
from jax import lax
from jax.experimental import pallas as pl
from jax.experimental.pallas import tpu as pltpu
from jax.sharding import Mesh
from jax.sharding import PartitionSpec as P

EXPERTS = 32
TOP = 2
MOE_DEV = 128
CAP = 16
PLANES = 16
CHUNKS = 2
EP_TP = ("ep_0", "ep_1", "ep_2", "tp")
EP = ("ep_0", "ep_1", "ep_2")
CHIPS = ("ep_0", "ep_1")
CORE_TP = ("ep_2", "tp")

epsilon = 1e-06
f32 = jnp.float32
bf16 = jnp.bfloat16


def ring_pairs(move):
    pairs = []
    for core in range(2):
        for x in range(4):
            to_core, to_x = move(core, x)
            pairs.append((core * 4 + x, to_core * 4 + to_x))
    return pairs


def weight_partner(core, x):
    return core, (((x - core) % 4 ^ 1) + core) % 4


def hidden_partner(core, x):
    return core, ((3 - (x - core) % 4) + core) % 4


def other_core(core, x):
    return 1 - core, x


def diagonal(core, x):
    return 1 - core, weight_partner(core, x)[1]


def swapped(value, move):
    return lax.ppermute(value, CORE_TP, ring_pairs(move))


def exchanged(blocks):
    return lax.all_to_all(blocks, CHIPS, split_axis=0, concat_axis=0, tiled=True)


def params(mib):
    return pltpu.CompilerParams(vmem_limit_bytes=mib << 20)


def cost(microseconds, mib):
    return pl.CostEstimate(
        flops=int(microseconds * 7e8), bytes_accessed=mib << 20, transcendentals=0
    )


def block_slots(info, core):
    picks = info[0:TOP, :].astype(jnp.int32)
    first, second = picks[0:1, :], picks[1:2, :]
    count = info.shape[1]
    experts = lax.broadcasted_iota(jnp.int32, (EXPERTS, count), 0)
    in_first, in_second = first == experts, second == experts
    named = jnp.where(in_first | in_second, 1.0, 0.0).astype(bf16)
    earlier = (
        lax.broadcasted_iota(jnp.int32, (count, count), 0)
        < lax.broadcasted_iota(jnp.int32, (count, count), 1)
    )
    before = jnp.dot(
        named, jnp.where(earlier, 1.0, 0.0).astype(bf16), preferred_element_type=f32
    )
    slots = []
    for pick, mask in ((first, in_first), (second, in_second)):
        position = jnp.sum(jnp.where(mask, before, 0.0), axis=0, keepdims=True)
        slot = (pick >> 1) * CAP + position.astype(jnp.int32)
        slots.append(jnp.where((pick & 1) == core, slot, -1))
    return slots


def dispatch_kernel(where, x_ref, info_ref, gain_ref, out_ref):
    width = 1024
    widened = x_ref[...].astype(f32)
    inverse = lax.rsqrt(jnp.mean(widened * widened, axis=-1, keepdims=True) + epsilon)
    slot_a, slot_b = block_slots(info_ref[...], where[1])
    slots = lax.broadcasted_iota(jnp.int32, (PLANES * CAP, MOE_DEV), 0)
    spread = jnp.where((slots == slot_a) | (slots == slot_b), 1.0, 0.0).astype(bf16)

    depth = out_ref.shape[2]
    first = 0 if depth == x_ref.shape[1] else where[7] * depth

    def piece(k, carry):
        cols = pl.ds(pl.multiple_of(first + k * width, width), width)
        normed = (x_ref[:, cols].astype(f32) * inverse * gain_ref[:, cols]).astype(bf16)
        rows = jnp.dot(spread, normed, preferred_element_type=f32).astype(bf16)
        out_ref[:, :, pl.ds(pl.multiple_of(k * width, width), width)] = rows.reshape(
            PLANES, CAP, width
        )
        return carry

    lax.fori_loop(0, depth // width, piece, 0)


def dispatch(where, rows, info, gain, whole_rows, out_depth):
    depth = rows.shape[1]
    row_block = lambda i, w: (w[0] * 2 + i, 0)
    return pl.pallas_call(
        dispatch_kernel,
        grid_spec=pltpu.PrefetchScalarGridSpec(
            num_scalar_prefetch=1,
            grid=(2,),
            in_specs=[
                pl.BlockSpec((MOE_DEV, depth), row_block if whole_rows else lambda i, w: (i, 0)),
                pl.BlockSpec((info.shape[0], MOE_DEV), lambda i, w: (0, w[0] * 2 + i)),
                pl.BlockSpec((1, depth), lambda i, w: (0, 0)),
            ],
            out_specs=pl.BlockSpec((PLANES, CAP, out_depth), lambda i, w: (0, i, 0)),
        ),
        out_shape=jax.ShapeDtypeStruct((PLANES, 2 * CAP, out_depth), bf16),
        cost_estimate=cost(6, 6),
        name="dispatch",
    )(where, rows, info, gain)


def hidden_kernel(where, low, high, gate_own, up_own, gate_part, up_part, out_ref, totals):
    step, steps = pl.program_id(0), pl.num_programs(0)
    width = gate_own.shape[1]

    @pl.when(step == 0)
    def _():
        totals[...] = jnp.zeros_like(totals)

    def add(block):
        for i, ref in enumerate((gate_own, up_own, gate_part, up_part)):
            totals[i] += jnp.dot(block, ref[...], preferred_element_type=f32)

    @pl.when(step < steps // 2)
    def _():
        add(low[...])

    @pl.when(step >= steps // 2)
    def _():
        add(high[...])

    @pl.when(step == steps - 1)
    def _():
        for i in range(2):
            value = jax.nn.silu(totals[2 * i]) * totals[2 * i + 1]
            out_ref[:, i * width : (i + 1) * width] = value.astype(bf16)


def hidden_units(where, low, high, gate_own, up_own, gate_part, up_part):
    depth, width = gate_own.shape
    rows = low.shape[0]
    step = 1024
    half = depth // step // 2
    if low is high:
        order = lambda k, w: k
        high_block = lambda k, w: (0, jnp.maximum(k, half))
    else:
        order = lambda k, w: lax.rem(k + w[7] * half, 2 * half)
        high_block = lambda k, w: (0, jnp.maximum(k - half, 0))
    weight = pl.BlockSpec((step, width), lambda k, w: (order(k, w), 0))
    return pl.pallas_call(
        hidden_kernel,
        grid_spec=pltpu.PrefetchScalarGridSpec(
            num_scalar_prefetch=1,
            grid=(2 * half,),
            in_specs=[
                pl.BlockSpec((rows, step), lambda k, w: (0, jnp.minimum(k, half - 1))),
                pl.BlockSpec((rows, step), high_block),
            ]
            + [weight] * 4,
            out_specs=pl.BlockSpec((rows, 2 * width), lambda k, w: (0, 0)),
            scratch_shapes=[pltpu.VMEM((4, rows, width), f32)],
        ),
        out_shape=jax.ShapeDtypeStruct((rows, 2 * width), bf16),
        cost_estimate=cost(10, 12),
        compiler_params=params(60 if low is high else 24),
        name="hidden",
    )(where, low, high, gate_own, up_own, gate_part, up_part)


def down_kernel(where, near, far, own_ref, part_a, part_b, out_ref):
    quarter = near.shape[1] // 2

    def run(weight):
        total = None
        for i in range(4):
            source = (near, far)[i // 2]
            values = source[:, (i % 2) * quarter : (i % 2 + 1) * quarter]
            rows = pl.ds(pl.multiple_of(where[2 + i] * quarter, quarter), quarter)
            product = jnp.dot(values, weight[rows, :], preferred_element_type=f32)
            total = product if total is None else total + product
        out_ref[...] = total.astype(bf16).reshape(out_ref.shape)

    @pl.when(pl.program_id(0) < 2)
    def _():
        run(own_ref)

    @pl.when(pl.program_id(0) == 2)
    def _():
        run(part_a)

    @pl.when(pl.program_id(0) == 3)
    def _():
        run(part_b)


def down_result(where, near, far, down_own, down_a, down_b):
    rows = near.shape[0]
    depth, width = down_own.shape
    step = width // 2
    whole = pl.BlockSpec(near.shape, lambda j, w: (0, 0))
    return pl.pallas_call(
        down_kernel,
        grid_spec=pltpu.PrefetchScalarGridSpec(
            num_scalar_prefetch=1,
            grid=(4,),
            in_specs=[
                whole,
                whole,
                pl.BlockSpec((depth, step), lambda j, w: (0, jnp.minimum(j, 1))),
                pl.BlockSpec((depth, step), lambda j, w: (0, 0)),
                pl.BlockSpec((depth, step), lambda j, w: (0, 0)),
            ],
            out_specs=pl.BlockSpec((PLANES, rows // PLANES, step), lambda j, w: (0, 0, j)),
        ),
        out_shape=jax.ShapeDtypeStruct((PLANES, rows // PLANES, 2 * width), bf16),
        cost_estimate=cost(5, 7),
        compiler_params=params(20),
        name="down",
    )(where, near, far, down_own, down_a, down_b)


def combine_kernel(where, info_ref, result_ref, own_slice, other_slice):
    half = own_slice.shape[1]
    info = info_ref[...]
    slot_a, slot_b = block_slots(info, where[1])
    slots = lax.broadcasted_iota(jnp.int32, (PLANES * CAP, MOE_DEV), 0)
    weights = jnp.where(slots == slot_a, info[2:3, :], 0.0) + jnp.where(
        slots == slot_b, info[3:4, :], 0.0
    )
    coarse = weights.astype(bf16)
    fine = weights - coarse.astype(f32)
    table = jnp.concatenate([coarse.astype(f32).T, fine.T], axis=0).astype(bf16)
    for part, ref in enumerate((own_slice, other_slice)):
        rows = result_ref[:, :, part * half : (part + 1) * half].reshape(PLANES * CAP, half)
        total = jnp.dot(table, rows, preferred_element_type=f32)
        ref[...] = (total[:MOE_DEV] + total[MOE_DEV:]).astype(ref.dtype)


def combine(where, info, returned, own_type):
    half = returned.shape[2] // 2
    out = pl.BlockSpec((MOE_DEV, half), lambda i, w: (i, 0))
    return pl.pallas_call(
        combine_kernel,
        grid_spec=pltpu.PrefetchScalarGridSpec(
            num_scalar_prefetch=1,
            grid=(2,),
            in_specs=[
                pl.BlockSpec((4, MOE_DEV), lambda i, w: (0, w[0] * 2 + i)),
                pl.BlockSpec((PLANES, CAP, 2 * half), lambda i, w: (0, i, 0)),
            ],
            out_specs=[out, out],
        ),
        out_shape=[jax.ShapeDtypeStruct((2 * MOE_DEV, half), t) for t in (own_type, bf16)],
        cost_estimate=cost(4, 4),
        compiler_params=params(12),
        name="combine",
    )(where, info, returned)


def total_kernel(where, keep, partner, sib, diag, out_ref):
    half = pl.program_id(0)

    def add(mine, theirs):
        out_ref[...] = (mine[...].astype(f32) + theirs[...].astype(f32)).astype(bf16)

    for own_place in range(2):
        for sib_place in range(2):

            @pl.when(((half == where[0]) == (own_place == 0)) & ((half == where[6]) == (sib_place == 0)))
            def _():
                add((keep, partner)[own_place], (sib, diag)[sib_place])


def total_rows(where, keep, partner, sib, diag):
    rows, width = keep.shape
    whole = pl.BlockSpec((rows, width), lambda i, w: (0, 0))
    return pl.pallas_call(
        total_kernel,
        grid_spec=pltpu.PrefetchScalarGridSpec(
            num_scalar_prefetch=1,
            grid=(2,),
            in_specs=[whole] * 4,
            out_specs=pl.BlockSpec((rows, width), lambda i, w: (i, 0)),
        ),
        out_shape=jax.ShapeDtypeStruct((2 * rows, width), bf16),
        cost_estimate=cost(3, 4),
        compiler_params=params(12),
        name="total",
    )(where, keep, partner, sib, diag)


def gated_rows(value, gate):
    return (value.astype(f32) * jax.nn.sigmoid(gate.astype(f32))).astype(bf16)


def conv_kernel(
    value_ref, gate_ref, halo_ref, taps_ref, gain_ref, bias_ref, top_ref, bottom_ref, rows, mixed
):
    reach = halo_ref.shape[0]
    block = value_ref.shape[0]
    lanes = 128

    @pl.when(pl.program_id(0) == 0)
    def _():
        rows[:reach, :] = halo_ref[...].astype(f32)

    @pl.when(pl.program_id(0) > 0)
    def _():
        rows[:reach, :] = rows[block:, :]

    rows[reach:, :] = gated_rows(value_ref[...], gate_ref[...]).astype(f32)

    def piece(k, carry):
        cols = pl.ds(pl.multiple_of(k * lanes, lanes), lanes)
        column = rows[:, cols]
        total = jnp.zeros((block, lanes), f32)
        for phase in range(8):
            moved = column if phase == 0 else pltpu.roll(column, phase, 0)
            for lag in range(phase, taps_ref.shape[0], 8):
                start = reach - (lag - phase)
                total = total + taps_ref[lag : lag + 1, cols] * moved[start : start + block]
        mixed[:, cols] = total
        return carry

    lax.fori_loop(0, mixed.shape[1] // lanes, piece, 0)
    whole = mixed[...]
    center = whole - jnp.mean(whole, axis=-1, keepdims=True)
    spread = jnp.mean(center * center, axis=-1, keepdims=True)
    scaled = center * lax.rsqrt(spread + epsilon) * gain_ref[...] + bias_ref[...]
    result = jax.nn.silu(scaled).astype(bf16)
    half = pl.num_programs(0) // 2

    @pl.when(pl.program_id(0) < half)
    def _():
        top_ref[...] = result

    @pl.when(pl.program_id(0) >= half)
    def _():
        bottom_ref[...] = result


def conv_rows(conv_value, conv_gate, earlier, conv_taps, conv_gain, conv_bias):
    length, width = conv_value.shape
    block = 64
    half = length // block // 2
    reach = earlier.shape[0]
    row_block = pl.BlockSpec((block, width), lambda i: (i, 0))
    whole = lambda rows: pl.BlockSpec((rows, width), lambda i: (0, 0))
    return pl.pallas_call(
        conv_kernel,
        grid=(length // block,),
        in_specs=[row_block, row_block, whole(reach), whole(conv_taps.shape[0]), whole(1), whole(1)],
        out_specs=[
            pl.BlockSpec((block, width), lambda i: (jnp.minimum(i, half - 1), 0)),
            pl.BlockSpec((block, width), lambda i: (jnp.maximum(i - half, 0), 0)),
        ],
        out_shape=[jax.ShapeDtypeStruct((length // 2, width), bf16)] * 2,
        scratch_shapes=[
            pltpu.VMEM((reach + block, width), f32),
            pltpu.VMEM((block, width), f32),
        ],
        cost_estimate=cost(14, 5),
        compiler_params=params(12),
    )(conv_value, conv_gate, earlier, conv_taps, conv_gain[None], conv_bias[None])


def work(
    conv_value,
    conv_gate,
    conv_taps,
    conv_gain,
    conv_bias,
    conv_projection,
    expert_input,
    expert_gain,
    route_experts,
    group_gate,
    expert_gate,
    gate_weight,
    up_weight,
    down_weight,
):
    core, x = lax.axis_index("ep_2"), lax.axis_index("tp")
    place = (x - core) % 4

    def half_of(which_core):
        spot = (x - which_core) % 4
        return ((spot == 1) | (spot == 2)).astype(jnp.int32)

    half, sib_half = half_of(core), half_of(1 - core)
    hidden_order = [place, place ^ 1, 3 - place, (3 - place) ^ 1]
    quarters = [(p + core) % 4 for p in hidden_order]
    where = jnp.stack([half, core, *quarters, sib_half, place >> 1]).astype(jnp.int32)
    rows_half = expert_input.shape[0] // 2
    gate_own, up_own, down_own = gate_weight[0], up_weight[0], down_weight[0]
    gain = expert_gain[None]

    outgoing = lax.dynamic_slice_in_dim(expert_input, sib_half * rows_half, rows_half, 0)
    sib_rows = swapped(outgoing, other_core)
    share = group_gate[:, None] * expert_gate / jnp.sum(expert_gate, axis=1, keepdims=True)
    info = jnp.concatenate([route_experts.astype(f32).T, share.T], axis=0)
    sib_info = swapped(info, other_core)
    gate_part = swapped(gate_own, weight_partner)
    up_part = swapped(up_own, weight_partner)

    infos = (info, sib_info)
    depth = expert_input.shape[1]
    first = dispatch(where, expert_input, route_experts.T, gain, True, depth // 2)
    first_arrived = exchanged(first)
    second = dispatch(where, sib_rows, sib_info, gain, False, depth)
    second, first_arrived = lax.optimization_barrier((second, first_arrived))
    second_arrived = exchanged(second).reshape(-1, depth)
    low = first_arrived.reshape(-1, depth // 2)
    high = swapped(low, hidden_partner)
    arrived = ((low, high), (second_arrived, second_arrived))

    reach = 32
    tail = gated_rows(conv_value[-reach:], conv_gate[-reach:])
    count = lax.axis_size(EP_TP)
    earlier = lax.ppermute(tail, EP_TP, [(k, k + 1) for k in range(count - 1)])
    conv_value, conv_gate, _ = lax.optimization_barrier((conv_value, conv_gate, first))
    top, bottom = conv_rows(
        conv_value, conv_gate, earlier, conv_taps, conv_gain, conv_bias
    )
    middle_out = down_own.shape[1] // 2
    down_a = swapped(down_own[:, :middle_out], weight_partner)
    down_b = swapped(down_own[:, middle_out:], weight_partner)

    combined = []
    for k in range(CHUNKS):
        near = hidden_units(where, *arrived[k], gate_own, up_own, gate_part, up_part)
        far = swapped(near, hidden_partner)
        result = down_result(where, near, far, down_own, down_a, down_b)
        returned = exchanged(result)
        combined.append(combine(where, infos[k], returned, (f32, bf16)[k]))
    keep, from_partner = combined[0][0], swapped(combined[0][1], weight_partner)
    from_sib = swapped(combined[1][0], other_core)
    from_diag = swapped(combined[1][1], diagonal)
    expert_out = total_rows(where, keep, from_partner, from_sib, from_diag)

    rows = conv_value.shape[0]
    middle = rows // 2
    right = [(k, (k + 1) % 4) for k in range(4)]
    left = [(k, (k - 1) % 4) for k in range(4)]

    def passed(value, pairs):
        return lax.ppermute(value, "tp", pairs)

    left_top = passed(top, right)
    right_bottom = passed(bottom, left)
    left_bottom = passed(bottom, right)
    right_top = passed(top, left)
    far_top = passed(left_top, right)
    far_bottom = passed(right_bottom, left)
    conv_out = jnp.zeros((4 * rows, conv_projection.shape[1]), bf16)
    for block, offset, start in (
        (top, 0, 0),
        (bottom, 0, middle),
        (left_top, 3, 0),
        (right_bottom, 1, middle),
        (left_bottom, 3, middle),
        (right_top, 1, 0),
        (far_top, 2, 0),
        (far_bottom, 2, middle),
    ):
        product = jnp.dot(block, conv_projection, preferred_element_type=f32).astype(bf16)
        conv_out = lax.dynamic_update_slice_in_dim(
            conv_out, product, (x + offset) % 4 * rows + start, 0
        )
    return (conv_out, expert_out)


def solution(mesh):
    finer = Mesh(mesh.devices.reshape(4, 4, 2, mesh.shape["tp"]), EP_TP)
    in_specs = (
        P(EP_TP, None),
        P(EP_TP, None),
        P(),
        P(),
        P(),
        P(None, "tp"),
        P(EP, None),
        P(),
        P(EP, None),
        P(EP),
        P(EP, None),
        P(EP, None, "tp"),
        P(EP, None, "tp"),
        P(EP, None, "tp"),
    )
    out_specs = (P(EP, "tp"), P(EP, "tp"))
    return jax.shard_map(work, mesh=finer, in_specs=in_specs, out_specs=out_specs, check_vma=False)
```
